32 devices in a mesh: grp: 2 (over y), sp: 4 (over z), tp: 4 (over x, core).
Axes of the slice: x: 2, y: 2, z: 4, core: 2. Of those that a mesh axis runs over, the one named last changes fastest.
Arguments:
- mix_in: bfloat16 [2048, 1536], P(('grp', 'sp'), 'tp'), parts along dimension 0, may hold values from -6 to 6
- resid_in: bfloat16 [2048, 2048], P(('grp', 'sp', 'tp')), parts along dimension 0, may hold values from -6 to 6
- doc_ids: int32 [2048], P(('grp', 'sp')), parts along dimension 0, may hold values from 0 to 1, never falling along the last dimension, each value on 1 to 768 neighbouring positions
- group_weight: bfloat16 [4, 384, 384], P('tp'), may hold values from -0.3125 to 0.3125
- pool_scale: float32 [1536], P('tp'), may hold values from 0.1 to 1.9
- out_weight: bfloat16 [1536, 2048], P('tp'), may hold values from -0.15625 to 0.15625
- norm_gain: float32 [2048], replicated, may hold values from 0.1 to 1.9
- expert_ids: int32 [2048, 2], P(('grp', 'sp', 'tp')), parts along dimension 0, may hold values from 0 to 15, as said below
- route_weights: float32 [2048, 2], P(('grp', 'sp', 'tp')), parts along dimension 0, may hold values from 0.1 to 1
- w_gate: bfloat16 [16, 2048, 512], P(('sp', 'tp')), may hold values from -0.125 to 0.125
- w_up: bfloat16 [16, 2048, 512], P(('sp', 'tp')), may hold values from -0.125 to 0.125
- w_down: bfloat16 [16, 512, 2048], P(('sp', 'tp')), may hold values from -0.25 to 0.25
Outputs:
- layer_out: bfloat16 [2048, 2048], P(('grp', 'sp', 'tp')), parts along dimension 0
The draws below stay inside these ranges and needn't reach their ends.
There are 2 independent parts, one for each index of `grp`. The reference program is written for one: setup_inputs(seed, part) draws one part's arguments, and reference() takes and returns one part's arrays. A program takes and returns all parts, laid end to end along the dimension named above; an argument that names none is the same for every part. Nothing has to cross between parts.
Inputs may be any that keep to these rules, and one draw needn't show every extreme that they name: `doc_ids`: document numbers never fall along the positions. `expert_ids`: each row names two different experts of one group of 4 consecutive experts. Among the rows of one device (aligned blocks of 64 rows) no expert is named more than 16 times; in every draw the experts of some group are each named exactly 16 times in every block.
All inputs are finite; a program needn't handle non-finite values.
Results may differ from the reference program's by a relative error of at most 0.012.
Values may be sent and summed in bfloat16 or wider, within the bound.
No kernel may reach another device: no remote copies, remote signals or barrier semaphores. Data moves between devices by JAX's collectives and lax.ppermute only.
A program may use at most 64 MiB of HBM per device.

```python
import math
import jax
import jax.numpy as jnp
import numpy as np
from jax import lax

D = 2048
GD = 384
FF = 512
POOL_GROUPS = 4
HALO = 16
EXPERT_GROUPS = 4
TOP_K = 2
MIX = 1536
SLICE = 64
TOKENS = 1024
EXPERTS = 16
EPG = 4
CAP = 16
DOCS = 2
SEG_MOST = 768


def block_order(subkey):
    return jax.random.permutation(subkey, SLICE)


def draw_expert_ids(key, part):
    blocks = TOKENS // SLICE
    busy_count = EPG * CAP // 2
    subkeys = jax.random.split(jax.random.fold_in(key, 11), 5)
    busy_group = jax.random.randint(subkeys[0], (), 0, EXPERT_GROUPS)
    spare_pick = jax.random.randint(subkeys[1], (blocks, SLICE), 0, EXPERT_GROUPS - 1)
    position = jnp.arange(SLICE, dtype=jnp.int32)[None, :]
    unshuffled = jnp.where(position < busy_count, busy_group, (busy_group + 1 + spare_pick) % EXPERT_GROUPS)
    row_order = jax.vmap(block_order)(jax.random.split(subkeys[2], blocks))
    row_group = jnp.take_along_axis(unshuffled, row_order, axis=1)
    onehot = (row_group[:, :, None] == jnp.arange(EXPERT_GROUPS, dtype=jnp.int32)[None, None, :]).astype(jnp.int32)
    row_rank = jnp.sum(onehot * (jnp.cumsum(onehot, axis=1) - 1), axis=2)
    first_shift = jax.random.randint(subkeys[3], (blocks, EXPERT_GROUPS), 0, EPG)
    second_shift = jax.random.randint(subkeys[4], (blocks, EXPERT_GROUPS), 0, EPG - 1)
    first_base = jnp.take_along_axis(first_shift, row_group, axis=1)
    second_extra = jnp.take_along_axis(second_shift, row_group, axis=1)
    first_pick = row_group * EPG + (row_rank + first_base) % EPG
    second_pick = row_group * EPG + (row_rank + first_base + 1 + second_extra) % EPG
    return jnp.stack([first_pick, second_pick], axis=-1).reshape(TOKENS, TOP_K).astype(jnp.int32)


def block_scale(stream_key, dims, shards, low, largest):
    level, own = 1.0, jax.random.fold_in(stream_key, 6)
    for dim, shards_of in shards:
        heights = jnp.exp(jax.random.uniform(jax.random.fold_in(own, dim), (shards_of,), jnp.float32, low / len(shards), largest / len(shards)))
        level = level * jnp.repeat(heights, dims[dim] // shards_of).reshape([-1 if axis == dim else 1 for axis in range(len(dims))])
    return level


def length_profile(number_of, total, most, skew):
    portions = [(1 << 20) // math.isqrt(rank ** skew) + 1 for rank in range(2, number_of + 1)]
    rest, holding = total - most - (number_of - 1), [1] * (number_of - 1)
    while rest > 0:
        candidates = [i for i in range(number_of - 1) if holding[i] < most]
        whole, budget = sum([portions[i] for i in candidates]), rest
        for i in candidates:
            extra = min(most - holding[i], max(1, budget * portions[i] // whole), rest)
            holding[i] = holding[i] + extra
            rest = rest - extra
    return np.array([most] + holding)


def ragged(own_key, amount, total, most, slope):
    if amount == 2:
        one = jax.random.randint(own_key, (), max(1, total - most), min(most, total - 1) + 1)
        return jnp.stack([one, total - one])
    tallies = jnp.asarray(length_profile(amount, total, most, slope), jnp.int32)
    pairs = (amount - 1) // 2
    source_of, sink = tallies[1:1 + 2 * pairs:2], tallies[2:2 + 2 * pairs:2]
    margin = jnp.minimum(source_of - 1, most - sink)
    moved = jax.random.randint(jax.random.fold_in(own_key, 1), (pairs,), 0, 1 << 20) % (margin + 1)
    tallies = tallies.at[1:1 + 2 * pairs:2].set(source_of - moved).at[2:2 + 2 * pairs:2].set(sink + moved)
    return tallies[jax.random.permutation(jax.random.fold_in(own_key, 2), amount)]


def scatter_about(stream_key, dims, deviation, most, cuts=(), kind=jnp.bfloat16):
    loudness = block_scale(stream_key, dims, cuts, -0.22, 0.18) if cuts else 1.0
    entries = jax.random.normal(stream_key, dims, jnp.float32) * deviation * loudness
    return jnp.minimum(jnp.maximum(entries, -most), most).astype(kind)


def setup_inputs(seed: int = 0, part: int = 0) -> dict:
    keys = jax.random.split(jax.random.key(seed), 13)
    part_splits = jax.random.split(jax.random.fold_in(keys[12], part), 13)
    return {
        "mix_in": scatter_about(part_splits[0], (TOKENS, MIX), 1.0, 6.0, ((0, 4), (1, 4))),
        "resid_in": scatter_about(part_splits[1], (TOKENS, D), 1.0, 6.0, ((0, 16),)),
        "doc_ids": jnp.searchsorted(jnp.cumsum(ragged(part_splits[2], DOCS, TOKENS, SEG_MOST, 2)), jnp.arange(TOKENS), side="right").astype(jnp.int32),
        "group_weight": scatter_about(keys[3], (POOL_GROUPS, GD, GD), GD ** -0.5, 0.3125, ((0, 4),)),
        "pool_scale": jnp.clip(1.0 + 0.18 * jax.random.normal(keys[4], (MIX,), jnp.float32), 0.1, 1.9),
        "out_weight": scatter_about(keys[5], (MIX, D), MIX ** -0.5, 0.15625, ((0, 4),)),
        "norm_gain": jnp.clip(1.0 + 0.18 * jax.random.normal(keys[6], (D,), jnp.float32), 0.1, 1.9),
        "expert_ids": draw_expert_ids(jax.random.fold_in(jax.random.fold_in(keys[12], part), 71), part),
        "route_weights": jnp.clip(jnp.exp(math.log(1.0) - 2.3025851 * jax.random.uniform(part_splits[8], (TOKENS, TOP_K), jnp.float32) ** block_scale(part_splits[8], (TOKENS, TOP_K), ((0, 16),), -0.2, 0.2)), 0.1, 1.0),
        "w_gate": scatter_about(keys[9], (EXPERTS, D, FF), D ** -0.5, 0.125, ((0, 16),)),
        "w_up": scatter_about(keys[10], (EXPERTS, D, FF), D ** -0.5, 0.125, ((0, 16),)),
        "w_down": scatter_about(keys[11], (EXPERTS, FF, D), FF ** -0.5, 0.25, ((0, 16),)),
    }


def expert_rows(flat_rows, gate_matrix, up_matrix, down_matrix):
    gate_part = jnp.dot(flat_rows, gate_matrix, preferred_element_type=jnp.float32)
    up_part = jnp.dot(flat_rows, up_matrix, preferred_element_type=jnp.float32)
    hidden = (jax.nn.silu(gate_part) * up_part).astype(jnp.bfloat16)
    return jnp.dot(hidden, down_matrix, preferred_element_type=jnp.float32).astype(jnp.bfloat16)

def reference(mix_in, resid_in, doc_ids, group_weight, pool_scale, out_weight, norm_gain, expert_ids, route_weights, w_gate, w_up, w_down):
    marked = doc_ids.astype(jnp.int32) + 1
    padded = jnp.concatenate([jnp.zeros((HALO, MIX), jnp.float32), mix_in.astype(jnp.float32)], axis=0)
    pad_marks = jnp.concatenate([jnp.zeros((HALO,), jnp.int32), marked])
    reach = jnp.left_shift(jnp.int32(2), jnp.arange(MIX, dtype=jnp.int32) // GD)
    running = jnp.zeros((TOKENS, MIX), jnp.float32)
    members = jnp.zeros((TOKENS, MIX), jnp.float32)
    for offset in range(HALO):
        rows_back = padded[HALO - offset:HALO - offset + TOKENS]
        same_doc = pad_marks[HALO - offset:HALO - offset + TOKENS] == marked
        keep = same_doc[:, None] & (offset < reach)[None, :]
        running = running + jnp.where(keep, rows_back, 0.0)
        members = members + keep.astype(jnp.float32)
    mixed = (running / members - mix_in.astype(jnp.float32)).astype(jnp.bfloat16)
    pieces = []
    for group_index in range(POOL_GROUPS):
        lower = group_index * GD
        product = jnp.dot(mixed[:, lower:lower + GD], group_weight[group_index], preferred_element_type=jnp.float32)
        pieces.append((product * pool_scale[lower:lower + GD]).astype(jnp.bfloat16))
    grouped = jnp.concatenate(pieces, axis=1)
    projected = jnp.dot(grouped, out_weight, preferred_element_type=jnp.float32)
    stream = (resid_in.astype(jnp.float32) + projected).astype(jnp.bfloat16)
    stream_f = stream.astype(jnp.float32)
    level = lax.optimization_barrier(jnp.mean(stream_f * stream_f, axis=1, keepdims=True))
    normed = (stream_f * lax.rsqrt(level + 1e-06) * norm_gain.astype(jnp.float32)).astype(jnp.bfloat16)
    route_total = TOKENS * TOP_K
    route_expert = expert_ids.reshape(-1).astype(jnp.int32)
    onehot = (route_expert[:, None] == jnp.arange(EXPERTS, dtype=jnp.int32)[None, :]).astype(jnp.int32)
    slot_index = lax.optimization_barrier(jnp.sum(onehot * (jnp.cumsum(onehot, axis=0) - 1), axis=1)).astype(jnp.int32)
    table = jnp.full((EXPERTS, EXPERTS * CAP), route_total, jnp.int32)
    table = table.at[route_expert, slot_index].set(jnp.arange(route_total, dtype=jnp.int32))
    normed_pad = jnp.concatenate([normed, jnp.zeros((1, D), jnp.bfloat16)], axis=0)

    def serve(answers, inputs):
        gate_matrix, up_matrix, down_matrix, routes = inputs
        rows_in = normed_pad[routes // TOP_K]
        served = expert_rows(rows_in, gate_matrix, up_matrix, down_matrix)
        return (answers.at[routes].set(served), None)
    answers, _ = lax.scan(serve, jnp.zeros((route_total + 1, D), jnp.bfloat16), (w_gate, w_up, w_down, table))
    weighted = answers[:route_total].astype(jnp.float32) * route_weights.reshape(-1)[:, None]
    paired = weighted.reshape(TOKENS, TOP_K, D)
    return (stream_f + paired[:, 0] + paired[:, 1]).astype(jnp.bfloat16)
```

```python
import jax
import jax.numpy as jnp
from jax import lax
from jax.sharding import PartitionSpec as P

HALO = 16
TOP_K = 2
EXPERT_GROUPS = 4
LANES = 128


def f32(value):
    return value.astype(jnp.float32)


def bf16(value):
    return value.astype(jnp.bfloat16)


def dot(left, right):
    return jnp.dot(left, right, preferred_element_type=jnp.float32)


def swap(value, axis, flip):
    return lax.ppermute(value, axis, [(i, i ^ flip) for i in range(lax.axis_size(axis))])


def mixer(mix_in, doc_ids, group_weight, pool_scale):
    local_rows, group_width = mix_in.shape
    sp_size = lax.axis_size("sp")
    reach = jnp.left_shift(jnp.int32(2), lax.axis_index("tp"))
    marks = f32(doc_ids + 1)[:, None]
    tail = jnp.concatenate(
        [
            mix_in[local_rows - HALO :],
            jnp.broadcast_to(bf16(marks[local_rows - HALO :]), (HALO, LANES)),
        ],
        axis=1,
    )
    prior = lax.ppermute(tail, "sp", [(i, i + 1) for i in range(sp_size - 1)])
    extended = f32(jnp.concatenate([prior[:, :group_width], mix_in], axis=0))
    ext_marks = jnp.concatenate([f32(prior[:, group_width : group_width + 1]), marks], axis=0)
    running = jnp.zeros((local_rows, group_width), jnp.float32)
    members = jnp.zeros((local_rows, 1), jnp.float32)
    for offset in range(HALO):
        window = slice(HALO - offset, HALO - offset + local_rows)
        keep = (ext_marks[window] == marks) & (offset < reach)
        running = running + jnp.where(keep, extended[window], 0.0)
        members = members + f32(keep)
    mixed = bf16(running / members - f32(mix_in))
    return bf16(dot(mixed, group_weight[0]) * pool_scale)


def project(grouped, out_weight):
    tp_size = lax.axis_size("tp")
    token_rows = grouped.shape[0] // tp_size
    own = lax.axis_index("tp")

    def part(flip):
        rows = lax.dynamic_slice_in_dim(grouped, (own ^ flip) * token_rows, token_rows, 0)
        return dot(rows, out_weight)

    sums = {flip: part(flip) for flip in range(tp_size)}
    half = 1
    while half < tp_size:
        flips = sorted(sums)
        for flip in flips:
            if flip & half:
                sums[flip ^ half] = sums[flip ^ half] + f32(swap(bf16(sums.pop(flip)), "tp", half))
        half *= 2
    return sums[0]


def experts_in_row(stream_f, normed, expert_ids, route_weights, w_gate, w_up, w_down):
    token_rows, width = normed.shape
    sp_size, tp_size = lax.axis_size("sp"), lax.axis_size("tp")
    group_rows = token_rows // 2
    here, lane = lax.axis_index("sp"), lax.axis_index("tp")
    relative = (expert_ids[:, 0] // tp_size) ^ here
    member = relative[:, None] == jnp.arange(sp_size, dtype=jnp.int32)[None, :]
    rank = jnp.sum(jnp.where(member, jnp.cumsum(member.astype(jnp.int32), axis=0) - 1, 0), axis=1)
    slot = relative * group_rows + rank
    pack = bf16(slot[None, :] == jnp.arange(sp_size * group_rows, dtype=jnp.int32)[:, None])
    column = jnp.arange(LANES, dtype=jnp.int32)[None, :]
    within = expert_ids % tp_size
    high = lax.reduce_precision(route_weights, 8, 7)
    low = route_weights - high
    notes = jnp.zeros((token_rows, LANES), jnp.float32)
    for visit in range(TOP_K):
        place = 2 * within[:, visit : visit + 1]
        notes = notes + jnp.where(column == place, high[:, visit : visit + 1], 0.0)
        notes = notes + jnp.where(column == place + 1, low[:, visit : visit + 1], 0.0)
    packed = bf16(dot(pack, jnp.concatenate([normed, bf16(notes)], axis=1)))
    held = {0: packed[:group_rows]}
    for flip in range(1, sp_size):
        held[flip] = swap(packed[flip * group_rows : (flip + 1) * group_rows], "sp", flip)
    back = []
    for flip in range(sp_size):
        rows = {0: held[flip]}
        half = tp_size // 2
        while half:
            for key in sorted(rows):
                rows[key ^ half] = swap(rows[key], "tp", half)
            half //= 2
        stacked = jnp.concatenate([rows[key] for key in range(tp_size)], axis=0)
        tokens = stacked[:, :width]
        labels = f32(stacked[:, width:])
        weight = jnp.sum(jnp.where(column // 2 == lane, labels, 0.0), axis=1, keepdims=True)
        hidden = bf16(jax.nn.silu(dot(tokens, w_gate[0])) * dot(tokens, w_up[0]))
        answer = dot(hidden, w_down[0]) * weight
        sums = {key: answer[key * group_rows : (key + 1) * group_rows] for key in range(tp_size)}
        half = 1
        while half < tp_size:
            for key in sorted(sums):
                if key & half:
                    sums[key ^ half] = sums[key ^ half] + f32(swap(bf16(sums.pop(key)), "tp", half))
            half *= 2
        total = bf16(sums[0])
        back.append(swap(total, "sp", flip) if flip else total)
    returned = jnp.concatenate(back, axis=0)
    gathered = lax.dot_general(
        pack, returned, (((0,), (0,)), ((), ())), preferred_element_type=jnp.float32
    )
    return bf16(stream_f + gathered)


def experts_direct(stream_f, normed, expert_ids, route_weights, w_gate, w_up, w_down):
    token_rows, width = normed.shape
    expert_count = lax.axis_size("sp") * lax.axis_size("tp")
    capacity = max(2, EXPERT_GROUPS * token_rows // expert_count)
    route_expert = expert_ids.reshape(-1)
    onehot = (route_expert[:, None] == jnp.arange(expert_count, dtype=jnp.int32)[None, :]).astype(
        jnp.int32
    )
    slot_index = jnp.sum(onehot * (jnp.cumsum(onehot, axis=0) - 1), axis=1)
    target = route_expert * capacity + slot_index
    source_rows = jnp.repeat(normed, TOP_K, axis=0)
    outbox = jnp.zeros((expert_count * capacity, width), jnp.bfloat16).at[target].set(source_rows)
    arrived = lax.all_to_all(
        outbox.reshape(expert_count, capacity, width),
        ("sp", "tp"),
        split_axis=0,
        concat_axis=0,
        tiled=True,
    )
    rows = arrived.reshape(-1, width)
    hidden = bf16(jax.nn.silu(dot(rows, w_gate[0])) * dot(rows, w_up[0]))
    served = bf16(dot(hidden, w_down[0])).reshape(arrived.shape)
    returned = lax.all_to_all(served, ("sp", "tp"), split_axis=0, concat_axis=0, tiled=True)
    answers = f32(returned.reshape(expert_count * capacity, width)[target])
    weighted = answers * route_weights.reshape(-1)[:, None]
    paired = weighted.reshape(token_rows, TOP_K, width)
    return bf16(stream_f + paired[:, 0] + paired[:, 1])


def shards(
    mix_in,
    resid_in,
    doc_ids,
    group_weight,
    pool_scale,
    out_weight,
    norm_gain,
    expert_ids,
    route_weights,
    w_gate,
    w_up,
    w_down,
):
    grouped = mixer(mix_in, doc_ids, group_weight, pool_scale)
    projected = project(grouped, out_weight)
    stream_f = f32(bf16(f32(resid_in) + projected))
    level = jnp.mean(stream_f * stream_f, axis=1, keepdims=True)
    normed = bf16(stream_f * lax.rsqrt(level + 1e-06) * norm_gain)
    sp_size = lax.axis_size("sp")
    one_row_per_group = sp_size == EXPERT_GROUPS and sp_size & (sp_size - 1) == 0
    experts = experts_in_row if one_row_per_group else experts_direct
    return experts(stream_f, normed, expert_ids, route_weights, w_gate, w_up, w_down)


def solution(mesh):
    return jax.shard_map(
        shards,
        mesh=mesh,
        in_specs=(
            P(("grp", "sp"), "tp"),
            P(("grp", "sp", "tp"), None),
            P(("grp", "sp")),
            P("tp", None, None),
            P("tp"),
            P("tp", None),
            P(),
            P(("grp", "sp", "tp"), None),
            P(("grp", "sp", "tp"), None),
            P(("sp", "tp"), None, None),
            P(("sp", "tp"), None, None),
            P(("sp", "tp"), None, None),
        ),
        out_specs=P(("grp", "sp", "tp"), None),
        check_vma=False,
    )
```

```python
import jax
import jax.numpy as jnp
from jax import lax
from jax.experimental import pallas as pl
from jax.experimental.pallas import tpu as pltpu
from jax.sharding import PartitionSpec as P

HALO = 16
TOP_K = 2
EXPERT_GROUPS = 4
LANES = 128


def f32(value):
    return value.astype(jnp.float32)


def bf16(value):
    return value.astype(jnp.bfloat16)


def dot(left, right):
    return jnp.dot(left, right, preferred_element_type=jnp.float32)


def swap(value, axis, flip):
    return lax.ppermute(value, axis, [(i, i ^ flip) for i in range(lax.axis_size(axis))])


def in_vmem(value):
    return pltpu.with_memory_space_constraint(value, pltpu.VMEM)


def struct(shape, dtype=jnp.bfloat16):
    return jax.ShapeDtypeStruct(shape, dtype)


def local_call(body, out_shape, flops, mib, *operands):
    return pl.pallas_call(
        body,
        out_shape=out_shape,
        cost_estimate=pl.CostEstimate(flops=flops, transcendentals=0, bytes_accessed=1 << 20),
        compiler_params=pltpu.CompilerParams(vmem_limit_bytes=mib << 20),
    )(*operands)


def halo_body(doc_ref, rows_ref, out_ref):
    group_width = rows_ref.shape[1]
    marks = jnp.broadcast_to(f32(doc_ref[:, doc_ref.shape[1] - LANES :] + 1), (HALO, LANES))
    out_ref[:, :group_width] = rows_ref[...]
    out_ref[:, group_width:] = bf16(pltpu.roll(marks, HALO, 1))


def mixer_body(tp_size, prior_ref, doc_ref, mix_ref, weight_ref, scale_ref, out_weight_ref, *outs):
    rows, group_width = mix_ref.shape
    token_rows = rows // tp_size
    grouped_ref = outs[-1]
    own = lax.axis_index("tp")
    reach = jnp.left_shift(jnp.int32(2), own)
    marks = jnp.broadcast_to(f32(doc_ref[...] + 1), (rows, rows))
    here = lax.broadcasted_iota(jnp.int32, (rows, rows), 0)
    there = lax.broadcasted_iota(jnp.int32, (rows, rows), 1)
    column = jnp.sum(jnp.where(here == there, marks, 0.0), axis=1, keepdims=True)
    band = (there <= here) & (there > here - reach) & (marks == column)
    band = jnp.where(band, 1.0, 0.0)
    before = lax.broadcasted_iota(jnp.int32, (rows, LANES), 1) - HALO
    place = lax.broadcasted_iota(jnp.int32, (rows, LANES), 0)
    prior_marks = f32(prior_ref[0:1, group_width:])
    early = (before < 0) & (before > place - reach) & (prior_marks == column)
    early = jnp.where(early, 1.0, 0.0)
    members = jnp.sum(band, axis=1, keepdims=True) + jnp.sum(early, axis=1, keepdims=True)
    prior_rows = jnp.concatenate(
        [prior_ref[:, :group_width], jnp.zeros((LANES - HALO, group_width), jnp.bfloat16)], axis=0
    )
    total = dot(bf16(band), mix_ref[...]) + dot(bf16(early), prior_rows)
    mixed = bf16(total / members - f32(mix_ref[...]))
    grouped_ref[...] = bf16(dot(mixed, weight_ref[0]) * scale_ref[...])
    for flip in sorted(range(tp_size), reverse=True):
        start = pl.multiple_of((own ^ flip) * token_rows, token_rows)
        part = dot(grouped_ref[pl.ds(start, token_rows), :], out_weight_ref[...])
        out_ref = outs[flip % 2]
        half = flip // 2
        out_ref[half * token_rows : (half + 1) * token_rows, :] = part.astype(out_ref.dtype)


def mixer_sums(mix_in, doc_ids, group_weight, pool_scale, out_weight):
    local_rows, group_width = mix_in.shape
    sp_size, tp_size = lax.axis_size("sp"), lax.axis_size("tp")
    token_rows = local_rows // tp_size
    width = out_weight.shape[1]
    docs = doc_ids.reshape(1, local_rows)
    tail = pl.pallas_call(
        halo_body,
        grid=(1,),
        in_specs=[
            pl.BlockSpec((1, local_rows), lambda i: (0, 0)),
            pl.BlockSpec((HALO, group_width), lambda i: (local_rows // HALO - 1, 0)),
        ],
        out_specs=pl.BlockSpec((HALO, group_width + LANES), lambda i: (0, 0)),
        out_shape=struct((HALO, group_width + LANES)),
        compiler_params=pltpu.CompilerParams(vmem_limit_bytes=1 << 20),
    )(docs, mix_in)
    prior = lax.ppermute(tail, "sp", [(i, i + 1) for i in range(sp_size - 1)])
    half_rows = local_rows // 2
    kept, sent = pl.pallas_call(
        lambda *refs: mixer_body(tp_size, *refs),
        out_shape=(struct((half_rows, width), jnp.float32), struct((half_rows, width))),
        scratch_shapes=[pltpu.VMEM((local_rows, group_width), jnp.bfloat16)],
        cost_estimate=pl.CostEstimate(
            flops=2 * local_rows * group_width * width, transcendentals=0, bytes_accessed=1 << 20
        ),
        compiler_params=pltpu.CompilerParams(vmem_limit_bytes=16 << 20),
    )(prior, docs, mix_in, group_weight, pool_scale.reshape(1, -1), out_weight)
    arrived = swap(sent, "tp", 1)
    kept = kept.reshape(2, token_rows, width)
    arrived = arrived.reshape(2, token_rows, width)
    far = swap(bf16(kept[1] + f32(arrived[1])), "tp", 2)
    return kept[0] + f32(arrived[0]) + f32(far)


def expert_body(lane_count, *refs):
    own = lax.axis_index("tp")
    pieces = refs[:lane_count]
    gate_ref, up_ref, down_ref, kept_ref, sent_ref = refs[lane_count:]
    width = gate_ref.shape[1]
    rows = pieces[0].shape[0]
    tokens = jnp.concatenate([piece[:, :width] for piece in pieces], axis=0)
    labels = f32(jnp.concatenate([piece[:, width:] for piece in pieces], axis=0))
    column = lax.broadcasted_iota(jnp.int32, labels.shape, 1)
    mine = (column == 2 * own) | (column == 2 * own + 1)
    weight = jnp.sum(jnp.where(mine, labels, 0.0), axis=1, keepdims=True)
    gate = dot(tokens, gate_ref[0])
    up = dot(tokens, up_ref[0])
    hidden = bf16(gate / (1.0 + jnp.exp(-gate)) * up)
    answer = dot(hidden, down_ref[0]) * weight
    for key in range(lane_count):
        out_ref = sent_ref if key % 2 else kept_ref
        place = slice(key // 2 * rows, (key // 2 + 1) * rows)
        out_ref[place, :] = answer[key * rows : (key + 1) * rows].astype(out_ref.dtype)


def experts_in_row(stream_f, normed, expert_ids, route_weights, w_gate, w_up, w_down):
    token_rows, width = normed.shape
    sp_size, tp_size = lax.axis_size("sp"), lax.axis_size("tp")
    group_rows = token_rows // 2
    here = lax.axis_index("sp")
    relative = (expert_ids[:, 0] // tp_size) ^ here
    member = relative[:, None] == jnp.arange(sp_size, dtype=jnp.int32)[None, :]
    rank = jnp.sum(jnp.where(member, jnp.cumsum(member.astype(jnp.int32), axis=0) - 1, 0), axis=1)
    slot = relative * group_rows + rank
    pack = bf16(slot[None, :] == jnp.arange(sp_size * group_rows, dtype=jnp.int32)[:, None])
    column = jnp.arange(LANES, dtype=jnp.int32)[None, :]
    within = expert_ids % tp_size
    high = lax.reduce_precision(route_weights, 8, 7)
    low = route_weights - high
    notes = jnp.zeros((token_rows, LANES), jnp.float32)
    for visit in range(TOP_K):
        place = 2 * within[:, visit : visit + 1]
        notes = notes + jnp.where(column == place, high[:, visit : visit + 1], 0.0)
        notes = notes + jnp.where(column == place + 1, low[:, visit : visit + 1], 0.0)
    packed = bf16(dot(pack, jnp.concatenate([normed, bf16(notes)], axis=1)))
    held = {0: packed[:group_rows]}
    for flip in range(1, sp_size):
        held[flip] = swap(packed[flip * group_rows : (flip + 1) * group_rows], "sp", flip)
    weights = [in_vmem(w_gate), in_vmem(w_up), in_vmem(w_down)]
    flops = 6 * tp_size * group_rows * width * w_down.shape[1]
    half_rows = tp_size * group_rows // 2
    back = []
    for flip in range(sp_size):
        rows = {0: held[flip], 2: swap(held[flip], "tp", 2)}
        for key in (0, 2):
            rows[key + 1] = swap(rows[key], "tp", 1)
        kept, sent = local_call(
            lambda *refs: expert_body(tp_size, *refs),
            (struct((half_rows, width), jnp.float32), struct((half_rows, width))),
            flops,
            16,
            *[rows[key] for key in range(tp_size)],
            *weights,
        )
        arrived = swap(sent, "tp", 1).reshape(2, group_rows, width)
        kept = kept.reshape(2, group_rows, width)
        far = swap(bf16(kept[1] + f32(arrived[1])), "tp", 2)
        total = bf16(kept[0] + f32(arrived[0]) + f32(far))
        back.append(swap(total, "sp", flip) if flip else total)
    returned = jnp.concatenate(back, axis=0)
    gathered = lax.dot_general(
        pack, returned, (((0,), (0,)), ((), ())), preferred_element_type=jnp.float32
    )
    return bf16(stream_f + gathered)


def experts_direct(stream_f, normed, expert_ids, route_weights, w_gate, w_up, w_down):
    token_rows, width = normed.shape
    expert_count = lax.axis_size("sp") * lax.axis_size("tp")
    capacity = max(2, EXPERT_GROUPS * token_rows // expert_count)
    route_expert = expert_ids.reshape(-1)
    onehot = (route_expert[:, None] == jnp.arange(expert_count, dtype=jnp.int32)[None, :]).astype(
        jnp.int32
    )
    slot_index = jnp.sum(onehot * (jnp.cumsum(onehot, axis=0) - 1), axis=1)
    target = route_expert * capacity + slot_index
    source_rows = jnp.repeat(normed, TOP_K, axis=0)
    outbox = jnp.zeros((expert_count * capacity, width), jnp.bfloat16).at[target].set(source_rows)
    arrived = lax.all_to_all(
        outbox.reshape(expert_count, capacity, width),
        ("sp", "tp"),
        split_axis=0,
        concat_axis=0,
        tiled=True,
    )
    rows = arrived.reshape(-1, width)
    hidden = bf16(jax.nn.silu(dot(rows, w_gate[0])) * dot(rows, w_up[0]))
    served = bf16(dot(hidden, w_down[0])).reshape(arrived.shape)
    returned = lax.all_to_all(served, ("sp", "tp"), split_axis=0, concat_axis=0, tiled=True)
    answers = f32(returned.reshape(expert_count * capacity, width)[target])
    weighted = answers * route_weights.reshape(-1)[:, None]
    paired = weighted.reshape(token_rows, TOP_K, width)
    return bf16(stream_f + paired[:, 0] + paired[:, 1])


def shards(
    mix_in,
    resid_in,
    doc_ids,
    group_weight,
    pool_scale,
    out_weight,
    norm_gain,
    expert_ids,
    route_weights,
    w_gate,
    w_up,
    w_down,
):
    projected = mixer_sums(mix_in, doc_ids, group_weight, pool_scale, out_weight)
    stream_f = f32(bf16(f32(resid_in) + projected))
    level = jnp.mean(stream_f * stream_f, axis=1, keepdims=True)
    normed = bf16(stream_f * lax.rsqrt(level + 1e-06) * norm_gain)
    sp_size = lax.axis_size("sp")
    one_row_per_group = sp_size == EXPERT_GROUPS and sp_size & (sp_size - 1) == 0
    experts = experts_in_row if one_row_per_group else experts_direct
    return experts(stream_f, normed, expert_ids, route_weights, w_gate, w_up, w_down)


def solution(mesh):
    return jax.shard_map(
        shards,
        mesh=mesh,
        in_specs=(
            P(("grp", "sp"), "tp"),
            P(("grp", "sp", "tp"), None),
            P(("grp", "sp")),
            P("tp", None, None),
            P("tp"),
            P("tp", None),
            P(),
            P(("grp", "sp", "tp"), None),
            P(("grp", "sp", "tp"), None),
            P(("sp", "tp"), None, None),
            P(("sp", "tp"), None, None),
            P(("sp", "tp"), None, None),
        ),
        out_specs=P(("grp", "sp", "tp"), None),
        check_vma=False,
    )
```

```python
import jax
import jax.numpy as jnp
from jax import lax
from jax.experimental import pallas as pl
from jax.experimental.pallas import tpu as pltpu
from jax.sharding import PartitionSpec as P


HALO = 16
TOP_K = 2
EXPERT_GROUPS = 4
LANES = 128
HALO_FLOPS = 1 << 32


def f32(value):
    return value.astype(jnp.float32)


def bf16(value):
    return value.astype(jnp.bfloat16)


def dot(left, right):
    return jnp.dot(left, right, preferred_element_type=jnp.float32)


def swap(value, axis, flip):
    return lax.ppermute(value, axis, [(i, i ^ flip) for i in range(lax.axis_size(axis))])


def in_vmem(value):
    return pltpu.with_memory_space_constraint(value, pltpu.VMEM)


def in_hbm(value):
    return pltpu.with_memory_space_constraint(value, pltpu.HBM)


def struct(shape, dtype=jnp.bfloat16):
    return jax.ShapeDtypeStruct(shape, dtype)


CHUNKS = (0, 2, 3, 1)


def kernel_call(body, out_shape, flops, mib, *operands):
    return pl.pallas_call(
        body,
        out_shape=out_shape,
        cost_estimate=pl.CostEstimate(flops=flops, transcendentals=0, bytes_accessed=1 << 20),
        compiler_params=pltpu.CompilerParams(vmem_limit_bytes=mib << 20),
    )(*operands)


def halo_body(doc_ref, mix_ref, out_ref, docs, rows, arrivals):
    local_rows, group_width = mix_ref.shape
    fetches = [
        pltpu.make_async_copy(doc_ref, docs, arrivals.at[0]),
        pltpu.make_async_copy(mix_ref.at[pl.ds(local_rows - HALO, HALO)], rows, arrivals.at[1]),
    ]
    for fetch in fetches:
        fetch.start()
    for fetch in fetches:
        fetch.wait()
    marks = jnp.broadcast_to(f32(docs[:, local_rows - LANES :] + 1), (HALO, LANES))
    out_ref[:, :group_width] = rows[...]
    out_ref[:, group_width:] = bf16(pltpu.roll(marks, HALO, 1))


def mixer_body(tp_size, prior_ref, doc_ref, mix_ref, weight_ref, scale_ref, out_weight_ref, *outs):
    rows, group_width = mix_ref.shape
    token_rows = rows // tp_size
    grouped_ref, tie_ref = outs[-1], outs[-2]
    tie_ref[...] = jnp.zeros(tie_ref.shape, tie_ref.dtype)
    own = lax.axis_index("tp")
    reach = jnp.left_shift(jnp.int32(2), own)
    marks = jnp.broadcast_to(f32(doc_ref[...] + 1), (rows, rows))
    here = lax.broadcasted_iota(jnp.int32, (rows, rows), 0)
    there = lax.broadcasted_iota(jnp.int32, (rows, rows), 1)
    column = jnp.sum(jnp.where(here == there, marks, 0.0), axis=1, keepdims=True)
    band = (there <= here) & (there > here - reach) & (marks == column)
    band = jnp.where(band, 1.0, 0.0)
    before = lax.broadcasted_iota(jnp.int32, (rows, LANES), 1) - HALO
    place = lax.broadcasted_iota(jnp.int32, (rows, LANES), 0)
    prior_marks = f32(prior_ref[0:1, group_width:])
    early = (before < 0) & (before > place - reach) & (prior_marks == column)
    early = jnp.where(early, 1.0, 0.0)
    members = jnp.sum(band, axis=1, keepdims=True) + jnp.sum(early, axis=1, keepdims=True)
    prior_rows = jnp.concatenate(
        [prior_ref[:, :group_width], jnp.zeros((LANES - HALO, group_width), jnp.bfloat16)], axis=0
    )
    total = dot(bf16(band), mix_ref[...]) + dot(bf16(early), prior_rows)
    mixed = bf16(total / members - f32(mix_ref[...]))
    grouped_ref[...] = bf16(dot(mixed, weight_ref[0]) * scale_ref[...])
    for flip in sorted(range(tp_size), reverse=True):
        start = pl.multiple_of((own ^ flip) * token_rows, token_rows)
        part = dot(grouped_ref[pl.ds(start, token_rows), :], out_weight_ref[...])
        outs[flip][...] = part.astype(outs[flip].dtype)


def mixer_sums(mix_in, doc_ids, group_weight, pool_scale, out_weight, expert_ids, route_weights):
    local_rows, group_width = mix_in.shape
    sp_size, tp_size = lax.axis_size("sp"), lax.axis_size("tp")
    token_rows = local_rows // tp_size
    width = out_weight.shape[1]
    docs = doc_ids.reshape(1, local_rows)
    tail = pl.pallas_call(
        halo_body,
        in_specs=[pl.BlockSpec(memory_space=pltpu.HBM)] * 2,
        out_shape=struct((HALO, group_width + LANES)),
        scratch_shapes=[
            pltpu.VMEM((1, local_rows), jnp.int32),
            pltpu.VMEM((HALO, group_width), jnp.bfloat16),
            pltpu.SemaphoreType.DMA((2,)),
        ],
        cost_estimate=pl.CostEstimate(flops=HALO_FLOPS, transcendentals=0, bytes_accessed=1 << 20),
        compiler_params=pltpu.CompilerParams(vmem_limit_bytes=1 << 20),
    )(in_hbm(docs), in_hbm(mix_in))
    prior = lax.ppermute(tail, "sp", [(i, i + 1) for i in range(sp_size - 1)])
    wide, narrow = struct((token_rows, width), jnp.float32), struct((token_rows, width))
    kept, near, far_kept, far, tie = pl.pallas_call(
        lambda *refs: mixer_body(tp_size, *refs),
        out_shape=(wide, narrow, wide, narrow, struct((8, LANES), jnp.float32)),
        scratch_shapes=[pltpu.VMEM((local_rows, group_width), jnp.bfloat16)],
        cost_estimate=pl.CostEstimate(
            flops=2 * local_rows * group_width * width, transcendentals=0, bytes_accessed=1 << 20
        ),
        compiler_params=pltpu.CompilerParams(vmem_limit_bytes=16 << 20),
    )(
        prior,
        in_vmem(docs),
        in_vmem(mix_in),
        in_vmem(group_weight),
        in_vmem(pool_scale.reshape(1, -1)),
        in_vmem(out_weight),
    )
    expert_ids, route_weights, _ = lax.optimization_barrier((expert_ids, route_weights, tie))
    far = swap(far, "tp", 1)
    near = swap(near, "tp", 1)
    far = swap(bf16(far_kept + f32(far)), "tp", 2)
    return kept + f32(near) + f32(far), expert_ids, route_weights


def expert_body(lane_count, *refs):
    own = lax.axis_index("tp")
    pieces = refs[:lane_count]
    gate_ref, up_ref, down_ref, kept_ref, sent_ref = refs[lane_count:]
    width = gate_ref.shape[1]
    rows = pieces[0].shape[0]
    tokens = jnp.concatenate([piece[:, :width] for piece in pieces], axis=0)
    labels = f32(jnp.concatenate([piece[:, width:] for piece in pieces], axis=0))
    column = lax.broadcasted_iota(jnp.int32, labels.shape, 1)
    mine = (column == 2 * own) | (column == 2 * own + 1)
    weight = jnp.sum(jnp.where(mine, labels, 0.0), axis=1, keepdims=True)
    gate = dot(tokens, gate_ref[0])
    up = dot(tokens, up_ref[0])
    hidden = bf16(gate / (1.0 + jnp.exp(-gate)) * up)
    answer = dot(hidden, down_ref[0]) * weight
    for key in range(lane_count):
        out_ref = sent_ref if key % 2 else kept_ref
        place = slice(key // 2 * rows, (key // 2 + 1) * rows)
        out_ref[place, :] = answer[key * rows : (key + 1) * rows].astype(out_ref.dtype)


def experts_in_row(stream_f, normed, expert_ids, route_weights, w_gate, w_up, w_down):
    token_rows, width = normed.shape
    sp_size, tp_size = lax.axis_size("sp"), lax.axis_size("tp")
    group_rows = token_rows // 2
    here = lax.axis_index("sp")
    relative = (expert_ids[:, 0] // tp_size) ^ here
    member = relative[:, None] == jnp.arange(sp_size, dtype=jnp.int32)[None, :]
    rank = jnp.sum(jnp.where(member, jnp.cumsum(member.astype(jnp.int32), axis=0) - 1, 0), axis=1)
    slot = relative * group_rows + rank
    pack = bf16(slot[None, :] == jnp.arange(sp_size * group_rows, dtype=jnp.int32)[:, None])
    column = jnp.arange(LANES, dtype=jnp.int32)[None, :]
    within = expert_ids % tp_size
    high = lax.reduce_precision(route_weights, 8, 7)
    low = route_weights - high
    notes = jnp.zeros((token_rows, LANES), jnp.float32)
    for visit in range(TOP_K):
        place = 2 * within[:, visit : visit + 1]
        notes = notes + jnp.where(column == place, high[:, visit : visit + 1], 0.0)
        notes = notes + jnp.where(column == place + 1, low[:, visit : visit + 1], 0.0)
    packed = bf16(dot(pack, jnp.concatenate([normed, bf16(notes)], axis=1)))
    held = {0: packed[:group_rows]}
    for flip in range(1, sp_size):
        held[flip] = swap(packed[flip * group_rows : (flip + 1) * group_rows], "sp", flip)
    weights = [in_vmem(w_gate), in_vmem(w_up), in_vmem(w_down)]
    flops = 6 * tp_size * group_rows * width * w_down.shape[1]
    half_rows = tp_size * group_rows // 2
    back = {}
    for flip in CHUNKS:
        rows = {0: held[flip], 2: swap(held[flip], "tp", 2)}
        rows[1] = swap(rows[0], "tp", 1)
        rows[3] = swap(rows[2], "tp", 1)
        kept, sent = kernel_call(
            lambda *refs: expert_body(tp_size, *refs),
            (struct((half_rows, width), jnp.float32), struct((half_rows, width))),
            flops,
            16,
            *[rows[key] for key in range(tp_size)],
            *weights,
        )
        arrived = swap(sent, "tp", 1).reshape(2, group_rows, width)
        kept = kept.reshape(2, group_rows, width)
        far = swap(bf16(kept[1] + f32(arrived[1])), "tp", 2)
        total = bf16(kept[0] + f32(arrived[0]) + f32(far))
        back[flip] = swap(total, "sp", flip) if flip else total
    returned = jnp.concatenate([back[flip] for flip in range(sp_size)], axis=0)
    gathered = lax.dot_general(
        pack, returned, (((0,), (0,)), ((), ())), preferred_element_type=jnp.float32
    )
    return bf16(stream_f + gathered)


def experts_direct(stream_f, normed, expert_ids, route_weights, w_gate, w_up, w_down):
    token_rows, width = normed.shape
    expert_count = lax.axis_size("sp") * lax.axis_size("tp")
    capacity = max(2, EXPERT_GROUPS * token_rows // expert_count)
    route_expert = expert_ids.reshape(-1)
    onehot = (route_expert[:, None] == jnp.arange(expert_count, dtype=jnp.int32)[None, :]).astype(
        jnp.int32
    )
    slot_index = jnp.sum(onehot * (jnp.cumsum(onehot, axis=0) - 1), axis=1)
    target = route_expert * capacity + slot_index
    source_rows = jnp.repeat(normed, TOP_K, axis=0)
    outbox = jnp.zeros((expert_count * capacity, width), jnp.bfloat16).at[target].set(source_rows)
    arrived = lax.all_to_all(
        outbox.reshape(expert_count, capacity, width),
        ("sp", "tp"),
        split_axis=0,
        concat_axis=0,
        tiled=True,
    )
    rows = arrived.reshape(-1, width)
    hidden = bf16(jax.nn.silu(dot(rows, w_gate[0])) * dot(rows, w_up[0]))
    served = bf16(dot(hidden, w_down[0])).reshape(arrived.shape)
    returned = lax.all_to_all(served, ("sp", "tp"), split_axis=0, concat_axis=0, tiled=True)
    answers = f32(returned.reshape(expert_count * capacity, width)[target])
    weighted = answers * route_weights.reshape(-1)[:, None]
    paired = weighted.reshape(token_rows, TOP_K, width)
    return bf16(stream_f + paired[:, 0] + paired[:, 1])


def row_is_group(sp_size):
    return sp_size == EXPERT_GROUPS


def shards(
    mix_in,
    resid_in,
    doc_ids,
    group_weight,
    pool_scale,
    out_weight,
    norm_gain,
    expert_ids,
    route_weights,
    w_gate,
    w_up,
    w_down,
):
    projected, expert_ids, route_weights = mixer_sums(
        mix_in, doc_ids, group_weight, pool_scale, out_weight, expert_ids, route_weights
    )
    stream_f = f32(bf16(f32(resid_in) + projected))
    level = jnp.mean(stream_f * stream_f, axis=1, keepdims=True)
    normed = bf16(stream_f * lax.rsqrt(level + 1e-06) * norm_gain)
    experts = experts_in_row if row_is_group(lax.axis_size("sp")) else experts_direct
    return experts(stream_f, normed, expert_ids, route_weights, w_gate, w_up, w_down)


def solution(mesh):
    return jax.shard_map(
        shards,
        mesh=mesh,
        in_specs=(
            P(("grp", "sp"), "tp"),
            P(("grp", "sp", "tp"), None),
            P(("grp", "sp")),
            P("tp", None, None),
            P("tp"),
            P("tp", None),
            P(),
            P(("grp", "sp", "tp"), None),
            P(("grp", "sp", "tp"), None),
            P(("sp", "tp"), None, None),
            P(("sp", "tp"), None, None),
            P(("sp", "tp"), None, None),
        ),
        out_specs=P(("grp", "sp", "tp"), None),
        check_vma=False,
    )
```
